128 devices in a mesh: grp: 4 (over y, x), ep: 32 (over z, core).
Axes of the slice: x: 2, y: 2, z: 16, core: 2. Of those that a mesh axis runs over, the one named last changes fastest.
The devices are a block of a 8x8x16 slice.
Arguments:
- tokens: bfloat16 [4096, 2048], P(('grp', 'ep')), parts along dimension 0, may hold values from -6 to 6
- routes: int32 [4096, 4], P(('grp', 'ep')), parts along dimension 0, may hold values from 0 to 31, all different within a row; in each aligned block of 32 rows (0 to 31, 32 to 63, ...) at most 8 rows name the same one
- in_gain: float32 [2048], replicated, may hold values from 0.1 to 1.9
- group_router: float32 [2048, 4], replicated, may hold values from -0.03125 to 0.03125
- expert_router: float32 [2048, 32], replicated, may hold values from -0.03125 to 0.03125
- w_gate: bfloat16 [32, 2048, 512], P('ep'), may hold values from -0.125 to 0.125
- w_up: bfloat16 [32, 2048, 512], P('ep'), may hold values from -0.125 to 0.125
- w_down: bfloat16 [32, 512, 2048], P('ep')
- out_gain: float32 [2048], P('ep'), may hold values from 0.1 to 1.9
Outputs:
- mixed_out: bfloat16 [4096, 2048], P('grp', 'ep'), parts along dimension 0
The draws below stay inside these ranges and needn't reach their ends.
There are 4 independent parts, one for each index of `grp`. The reference program is written for one: setup_inputs(seed, part) draws one part's arguments, and reference() takes and returns one part's arrays. A program takes and returns all parts, laid end to end along the dimension named above; an argument that names none is the same for every part. Nothing has to cross between parts.
Inputs may be any that keep to these rules, and one draw needn't show every extreme that they name: `routes`: each row names 4 different experts; in the rows of one device no expert is named more than 8 times, a bound that some block reaches.
All inputs are finite; a program needn't handle non-finite values.
Results may differ from the reference program's by a relative error of at most 0.0085.
Values may be sent and summed in bfloat16 or wider, within the bound.
A program may use at most 64 MiB of HBM per device.

```python
import math
import jax
import jax.numpy as jnp
import numpy as np
from jax import lax

D = 2048
FF = 512
N_GROUPS = 4
TOPK = 4
TOK_DEV = 32
EXPERTS = 32
TOKENS = 1024
CAP = 8
N_EP = 32


def draw_w_down(key, part):
    first, second = jax.random.split(jax.random.fold_in(key, 7))
    column = jnp.arange(D, dtype=jnp.float32) / D
    base = jax.random.normal(first, (EXPERTS, FF, D), jnp.float32)
    rising = (1.0 + 2.0 * column) ** 0.5
    rough = jax.random.uniform(second, (D,), jnp.float32, 0.6, 1.4)
    return (base * FF ** (-0.5) * rising * rough).astype(jnp.bfloat16)


def block_scale(stream_key, shape, cuts, smallest, top_value):
    gain, own = 1.0, jax.random.fold_in(stream_key, 6)
    for axis_at, shards_of in cuts:
        steps = jnp.exp(jax.random.uniform(jax.random.fold_in(own, axis_at), (shards_of,), jnp.float32, smallest / len(cuts), top_value / len(cuts)))
        gain = gain * jnp.repeat(steps, shape[axis_at] // shards_of).reshape([-1 if axis == axis_at else 1 for axis in range(len(shape))])
    return gain


def shared_out(key, own, number, rows, count, top, bound, slope):
    order = jax.random.permutation(key, count)
    packed, usual = portions_of(count, rows * top, bound, slope, True), portions_of(count, rows * top, bound, slope, False)
    places = jnp.arange(count)

    def named(lengths, offset_by):
        used = int((lengths > 0).sum())
        fixed = max(1, used // 4)
        shifted = fixed + (places - fixed + offset_by * (used - fixed)) % max(1, count - fixed)
        return jnp.zeros((count,), jnp.int32).at[order[jnp.where(places < fixed, places, shifted)]].set(jnp.asarray(lengths, jnp.int32))

    lengths = jnp.where(number % 4 == 0, named(packed, number // 4), named(usual, number - number // 4 - 1))
    mixed = jax.random.permutation(jax.random.fold_in(own, 3), count)
    source_of, sink = mixed[0:count // 2 * 2:2], mixed[1:count // 2 * 2:2]
    room = jnp.minimum(lengths[source_of] - 1, bound - lengths[sink]) // 2
    room = jnp.where((source_of == order[0]) | (sink == order[0]) | (lengths[sink] == 0), 0, jnp.maximum(room, 0))
    shifted = jax.random.randint(jax.random.fold_in(own, 4), (count // 2,), 0, 1 << 20) % (room + 1)
    lengths = lengths.at[source_of].add(-shifted).at[sink].add(shifted)
    items = jnp.searchsorted(jnp.cumsum(lengths), jnp.arange(rows * top), side="right").astype(jnp.int32)
    table = items.reshape(top, rows).T
    table = table[jax.random.permutation(jax.random.fold_in(own, 1), rows)]
    offset_by = jax.random.randint(jax.random.fold_in(own, 2), (rows, 1), 0, top)
    return jnp.take_along_axis(table, (jnp.arange(top)[None, :] + offset_by) % top, axis=1)


def portions_of(number_of, total, reach, skew, full):
    loads = [(1 << 20) // math.isqrt(grade ** skew) + 1 for grade in range(1, number_of + 1)]
    largest = reach if full else min(reach, max(-(-total // number_of), total * loads[0] // sum(loads)))
    least = 1 if total - largest >= number_of - 1 else 0
    holding, surplus = [largest] + [least] * (number_of - 1), total - largest - least * (number_of - 1)
    while surplus > 0:
        movable = [i for i in range(1, number_of) if holding[i] < largest] or [i for i in range(1, number_of) if holding[i] < reach]
        mass, budget = sum([loads[i] for i in movable]), surplus
        for i in movable:
            addition = min(reach - holding[i], max(1, budget * loads[i] // mass), surplus)
            holding[i] = holding[i] + addition
            surplus = surplus - addition
    return np.array(holding)


def bell_draw(rng, shape, deviation, most, pieces=(), kind=jnp.bfloat16):
    level = block_scale(rng, shape, pieces, -0.22, 0.18) if pieces else 1.0
    array = jax.random.normal(rng, shape, jnp.float32) * deviation * level
    return jnp.minimum(jnp.maximum(array, -most), most).astype(kind)


def setup_inputs(seed: int = 0, part: int = 0) -> dict:
    key_of = jax.random.split(jax.random.key(seed), 10)
    part_splits = jax.random.split(jax.random.fold_in(key_of[9], part), 10)
    tokens = bell_draw(part_splits[0], (TOKENS, D), 1.0, 6.0, ((0, 32),))
    routes_keys = jax.random.split(jax.random.fold_in(part_splits[1], 1), TOKENS // TOK_DEV)
    routes_turns = jax.random.permutation(jax.random.fold_in(part_splits[1], 3), TOKENS // TOK_DEV)
    routes = jax.vmap(lambda own, number: shared_out(jax.random.fold_in(part_splits[1], 2), own, number, TOK_DEV, EXPERTS, TOPK, CAP, 2))(routes_keys, routes_turns).reshape((TOKENS, TOPK))
    in_gain = jnp.clip(1.0 + 0.18 * jax.random.normal(key_of[2], (D,), jnp.float32), 0.1, 1.9)
    group_router = bell_draw(key_of[3], (D, N_GROUPS), (16 * D) ** -0.5, 0.03125, (), jnp.float32)
    expert_router = bell_draw(key_of[4], (D, EXPERTS), (16 * D) ** -0.5, 0.03125, (), jnp.float32)
    w_gate = bell_draw(key_of[5], (EXPERTS, D, FF), D ** -0.5, 0.125, ((0, 32),))
    w_up = bell_draw(key_of[6], (EXPERTS, D, FF), D ** -0.5, 0.125, ((0, 32),))
    w_down = draw_w_down(jax.random.fold_in(key_of[9], 71), part)
    out_gain = jnp.clip(1.0 + 0.18 * jax.random.normal(key_of[8], (D,), jnp.float32), 0.1, 1.9)
    return {"tokens": tokens, "routes": routes, "in_gain": in_gain, "group_router": group_router, "expert_router": expert_router, "w_gate": w_gate, "w_up": w_up, "w_down": w_down, "out_gain": out_gain}


EPSILON = 1e-06

def expert_rows(rows, gate_mat, up_mat, down_mat):
    gate = jnp.dot(rows, gate_mat, preferred_element_type=jnp.float32)
    upward = jnp.dot(rows, up_mat, preferred_element_type=jnp.float32)
    hidden = (jax.nn.silu(gate) * upward).astype(jnp.bfloat16)
    return jnp.dot(hidden, down_mat, preferred_element_type=jnp.float32).astype(jnp.bfloat16)

def reference(tokens, routes, in_gain, group_router, expert_router, w_gate, w_up, w_down, out_gain):
    values = tokens.astype(jnp.float32)
    normed = (values * lax.rsqrt(lax.optimization_barrier(jnp.mean(values * values, axis=1, keepdims=True)) + EPSILON) * in_gain).astype(jnp.bfloat16)
    wide = normed.astype(jnp.float32)
    group_logit = jnp.dot(wide, group_router, precision=lax.Precision.HIGHEST)
    expert_logit = jnp.dot(wide, expert_router, precision=lax.Precision.HIGHEST)
    group_prob = jnp.exp(group_logit) / lax.optimization_barrier(jnp.sum(jnp.exp(group_logit), axis=1, keepdims=True))
    chosen = jnp.exp(jnp.take_along_axis(expert_logit, routes, axis=1))
    expert_prob = chosen / lax.optimization_barrier(jnp.sum(chosen, axis=1, keepdims=True))
    per_group = EXPERTS // N_GROUPS
    weight = jnp.take_along_axis(group_prob, routes // per_group, axis=1) * expert_prob
    pairs = routes.reshape(N_EP, TOK_DEV * TOPK)
    onehot = (pairs[:, :, None] == jnp.arange(EXPERTS, dtype=jnp.int32)).astype(jnp.int32)
    order_in = lax.optimization_barrier(jnp.sum(onehot * (jnp.cumsum(onehot, axis=1) - 1), axis=2)).astype(jnp.int32)
    slot_index = (jnp.arange(N_EP, dtype=jnp.int32)[:, None] * CAP + order_in).reshape(-1)
    expert_of = routes.reshape(-1)
    token_index = jnp.arange(TOKENS * TOPK, dtype=jnp.int32) // TOPK
    table = jnp.zeros((EXPERTS, N_EP * CAP), jnp.int32).at[expert_of, slot_index].set(token_index)
    answers = lax.map(lambda group: expert_rows(normed[group[0]], group[1], group[2], group[3]), (table, w_gate, w_up, w_down))
    pair_rows = answers[expert_of, slot_index].astype(jnp.float32)
    mixed = lax.optimization_barrier(jnp.sum((pair_rows * weight.reshape(-1)[:, None]).reshape(TOKENS, TOPK, D), axis=1))
    scale = lax.rsqrt(lax.optimization_barrier(jnp.mean(mixed * mixed, axis=1, keepdims=True)) + EPSILON)
    return (mixed * scale * out_gain).astype(jnp.bfloat16)
```

```python
import functools

import jax
import jax.numpy as jnp
from jax import lax
from jax.experimental import pallas as pl
from jax.experimental.pallas import tpu as pltpu
from jax.sharding import PartitionSpec as P

EPSILON = 1e-06
MESH = pl.DeviceIdType.MESH
F32 = jnp.float32
BF16 = jnp.bfloat16
LANES = 128


def layer_kernel(
    n_ep,
    tok_hbm, routes_hbm, gain_hbm, gr_hbm, er_hbm, wg_hbm, wu_hbm, wd_hbm, og_hbm,
    out_ref,
    tok, rts, gain, rtr, og, wg, wu, wd,
    own, oth, own_w, oth_w,
    gate_s, hid_s, y_own, y_snd, y_rcv,
    rs_s, rs_r, mix, mix_t, stat, total,
    in_sem, w_sem,
    ag_recv, agw_recv, dd_recv, ddw_recv, y_recv, rs_recv, mix_recv, stat_recv, tot_recv,
    ag_send, agw_send, dd_send, ddw_send, y_send, rs_send, mix_send, stat_send, tot_send,
):
    chips = n_ep // 2
    half = chips // 2
    rows, width = tok.shape
    experts = n_ep
    me = lax.axis_index("ep")
    z, c = me // 2, me % 2
    right, left = (me + 2) % n_ep, (me + n_ep - 2) % n_ep
    partner = me + 1 - 2 * c
    sides = (right, left)

    def remote(src, dst, send, recv, to):
        return pltpu.make_async_remote_copy(
            src_ref=src, dst_ref=dst, send_sem=send, recv_sem=recv,
            device_id={"ep": to}, device_id_type=MESH,
        )

    def wait(ref, sem):
        pltpu.make_async_copy(ref, ref, sem).wait()

    barrier = pltpu.get_barrier_semaphore()
    for peer in (right, left, partner):
        pl.semaphore_signal(barrier, inc=1, device_id={"ep": peer}, device_id_type=MESH)

    first = [(tok_hbm, tok), (gain_hbm, gain)]
    second = [
        (er_hbm, rtr.at[pl.ds(0, experts)]),
        (gr_hbm, rtr.at[pl.ds(experts, gr_hbm.shape[0])]),
        (routes_hbm, rts),
        (og_hbm, og),
    ]
    loads = [pltpu.make_async_copy(s, d, in_sem.at[i]) for i, (s, d) in enumerate(first + second)]
    for copy in loads:
        copy.start()
    big = [
        pltpu.make_async_copy(s, d, w_sem.at[i])
        for i, (s, d) in enumerate([(wg_hbm, wg), (wu_hbm, wu), (wd_hbm, wd)])
    ]
    for copy in big:
        copy.start()

    loads[0].wait()
    loads[1].wait()
    values = tok[...].astype(F32)
    scaled = values * lax.rsqrt(jnp.mean(values * values, axis=1, keepdims=True) + EPSILON)
    own[z] = (scaled * gain[...]).astype(BF16)
    pl.semaphore_wait(barrier, 3)

    subs = 4

    def piece(ref, slot, sub):
        a, b = sub // 2, sub % 2
        return ref.at[slot, pl.ds(a * (rows // 2), rows // 2), pl.ds(b * (width // 2), width // 2)]

    def slot_of(side, step):
        return (z + chips - step) % chips if side == 0 else (z + step) % chips

    def has_piece(side, step, sub):
        return step < half or (sub < subs // 2) == (side == 0)

    def forward(side, step, sub):
        slot = slot_of(side, step)
        remote(
            piece(own, slot, sub), piece(own, slot, sub),
            ag_send, ag_recv.at[side, step, sub], sides[side],
        ).start()

    def forward_w(side, step):
        slot = slot_of(side, step)
        remote(own_w.at[slot], own_w.at[slot], agw_send, agw_recv.at[side, step], sides[side]).start()

    def across(slot):
        remote(own.at[slot], oth.at[slot], dd_send, dd_recv.at[slot], partner).start()

    def across_w(slot):
        remote(own_w.at[slot], oth_w.at[slot], ddw_send, ddw_recv.at[slot], partner).start()

    for sub in range(subs):
        for side in range(2):
            forward(side, 0, sub)
    across(z)

    for copy in loads[2:]:
        copy.wait()
    mine = own[z]
    table = rtr[...]
    row_id = lax.broadcasted_iota(jnp.int32, table.shape, 0)
    table = jnp.where(row_id < experts + gr_hbm.shape[0], table, 0.0)
    high = table.astype(BF16)
    rest = table - high.astype(F32)
    middle = rest.astype(BF16)
    low = (rest - middle.astype(F32)).astype(BF16)
    repeats = LANES // rows
    wide = jnp.concatenate([mine] * repeats, axis=0)
    dims = (((1,), (1,)), ((), ()))
    logit = sum(
        lax.dot_general(part, wide, dims, preferred_element_type=F32) for part in (low, middle, high)
    )
    groups = gr_hbm.shape[0]
    per_group = experts // groups
    expert_exp = jnp.exp(logit[:experts])
    group_exp = jnp.exp(logit[experts:experts + groups])
    group_prob = group_exp / jnp.sum(group_exp, axis=0, keepdims=True)
    group_wide = jnp.concatenate(
        [jnp.broadcast_to(group_prob[g:g + 1], (per_group, LANES)) for g in range(groups)], axis=0
    )
    top = rts.shape[0]
    spread = (
        lax.broadcasted_iota(jnp.int32, (rows, LANES), 1) % rows
        == lax.broadcasted_iota(jnp.int32, (rows, LANES), 0)
    )
    chosen = jnp.dot(
        rts[...].astype(F32).astype(BF16), spread.astype(F32).astype(BF16), preferred_element_type=F32
    )
    expert_id = lax.broadcasted_iota(jnp.int32, (experts, LANES), 0).astype(F32)
    named = expert_id == chosen[0:1]
    for j in range(1, top):
        named = named | (expert_id == chosen[j:j + 1])
    picked = jnp.where(named, expert_exp, 0.0)
    weight = group_wide * (picked / jnp.sum(picked, axis=0, keepdims=True))
    lane_block = lax.broadcasted_iota(jnp.int32, (8, LANES), 1) // rows
    packed = weight[0:8]
    for g in range(1, experts // 8):
        packed = jnp.where(lane_block == g, weight[8 * g:8 * g + 8], packed)
    own_w[z] = packed
    for copy in big:
        copy.wait()
    for side in range(2):
        forward_w(side, 0)
    across_w(z)

    def weight_column(ref, slot):
        line = ref[slot, pl.ds(me % 8, 1), :]
        lane = lax.broadcasted_iota(jnp.int32, (rows, LANES), 1)
        token = lax.broadcasted_iota(jnp.int32, (rows, LANES), 0)
        hit = lane == token + rows * (me // 8)
        return jnp.sum(jnp.where(hit, jnp.broadcast_to(line, (rows, LANES)), 0.0), axis=1, keepdims=True)

    def slots_of(step):
        if step == 0 or step == half:
            return [slot_of(0, step)]
        return [slot_of(0, step), slot_of(1, step)]

    def block(step):
        slots = slots_of(step)
        count = 2 * len(slots) * rows

        def tokens_in():
            return jnp.concatenate([own[k] for k in slots] + [oth[k] for k in slots], axis=0)

        def part_gate():
            for k in slots:
                wait(oth.at[k], dd_recv.at[k])
            gate_s[pl.ds(0, count)] = jnp.dot(tokens_in(), wg[0], preferred_element_type=F32)

        def part_up():
            for k in slots:
                wait(oth_w.at[k], ddw_recv.at[k])
            upward = jnp.dot(tokens_in(), wu[0], preferred_element_type=F32)
            gate = gate_s[pl.ds(0, count)]
            column = jnp.concatenate(
                [weight_column(own_w, k) for k in slots] + [weight_column(oth_w, k) for k in slots], axis=0
            )
            hidden = gate / (1.0 + jnp.exp(-gate)) * upward
            hid_s[pl.ds(0, count)] = (hidden * column).astype(BF16)

        def part_down(b):
            cols = pl.ds(b * (width // 2), width // 2)
            y = jnp.dot(hid_s[pl.ds(0, count)], wd[0, :, cols], preferred_element_type=F32)
            for i, k in enumerate(slots):
                y_own[k, :, cols] = y[i * rows:(i + 1) * rows]
                j = i + len(slots)
                y_snd[k, :, cols] = y[j * rows:(j + 1) * rows].astype(BF16)
            if b == 1:
                for k in slots:
                    remote(y_snd.at[k], y_rcv.at[k], y_send, y_recv, partner).start()

        return [part_gate, part_up, lambda: part_down(0), lambda: part_down(1)]

    for step in range(1, half + 1):
        work = block(step - 1)
        for sub in range(subs):
            for side in range(2):
                if has_piece(side, step, sub):
                    slot = slot_of(side, step)
                    wait(piece(own, slot, sub), ag_recv.at[side, step - 1, sub])
                    if step < half and has_piece(side, step + 1, sub):
                        forward(side, step, sub)
            if sub == subs - 1:
                for side in range(2):
                    if step < half or side == 0:
                        slot = slot_of(side, step)
                        wait(own_w.at[slot], agw_recv.at[side, step - 1])
                        if step < half - 1 or (step == half - 1 and side == 0):
                            forward_w(side, step)
                        across(slot)
                        across_w(slot)
            work[sub]()
    for part in block(half):
        part()
    wait(y_rcv, y_recv)

    group_slots = chips // subs

    def mine_of(dest, sub):
        at = pl.ds(sub * group_slots, group_slots)
        cols = pl.ds(pl.multiple_of(dest * LANES, LANES), LANES)
        return y_own[at, :, cols] + y_rcv[at, :, cols].astype(F32)

    def buffer_of(side, step, sub):
        return (side * half + step) * subs + sub

    def starts(side, sub):
        return (sub < subs // 2) == (side == 0)

    for step in range(half):
        for turn in range(subs):
            for side in range(2):
                sub = (turn + (subs // 2) * (side + (step > 0))) % subs
                if step == 0 and not starts(side, sub):
                    continue
                dest = (z + half - step) % chips if side == 0 else (z + half + step) % chips
                value = mine_of(dest, sub)
                if step > 1 or (step == 1 and starts(side, sub)):
                    before = buffer_of(side, step - 1, sub)
                    wait(rs_r.at[before], rs_recv.at[before])
                    value = value + rs_r[before].astype(F32)
                at = buffer_of(side, step, sub)
                rs_s[at] = value.astype(BF16)
                remote(rs_s.at[at], rs_r.at[at], rs_send, rs_recv.at[at], sides[side]).start()

    lines = []
    for turn in range(subs):
        sub = (turn + subs // 2) % subs
        value = mine_of(z, sub)
        for side in range(2):
            last = buffer_of(side, half - 1, sub)
            wait(rs_r.at[last], rs_recv.at[last])
            value = value + rs_r[last].astype(F32)
        mix[c, pl.ds(sub * group_slots, group_slots)] = value
        flat = value.reshape(group_slots * rows, LANES)
        stat[z, pl.ds(sub, 1), :] = jnp.sum(jnp.transpose(flat * flat), axis=0, keepdims=True)

    remote(mix.at[c], mix.at[c], mix_send, mix_recv, partner).start()
    for hop in range(1, chips):
        to = (me + 2 * hop) % n_ep
        remote(stat.at[z], stat.at[z], stat_send, stat_recv, to).start()

    wait(mix.at[1 - c], mix_recv)
    feats = out_ref.shape[0]
    for sub in range(subs):
        flat = jnp.concatenate(
            [mix[h, sub * group_slots + j] for j in range(group_slots) for h in range(2)], axis=0
        )
        turned = jnp.transpose(flat)
        mix_t[:, pl.ds(sub * 2 * LANES, 2 * LANES)] = jnp.where(c == 0, turned[:feats], turned[feats:])
    eye = (
        lax.broadcasted_iota(jnp.int32, (feats, feats), 0)
        == lax.broadcasted_iota(jnp.int32, (feats, feats), 1)
    )
    out_gain = jnp.sum(
        jnp.where(eye, jnp.broadcast_to(og[...], (feats, feats)), 0.0), axis=1, keepdims=True
    )

    wait(stat.at[pl.ds(0, chips - 1)], stat_recv)
    total[c] = jnp.sum(stat[...], axis=0)
    remote(total.at[c], total.at[c], tot_send, tot_recv, partner).start()
    wait(total.at[1 - c], tot_recv)
    scale = lax.rsqrt(total[...] / width + EPSILON)
    s0, s1 = scale[0], scale[1]
    spot = lax.broadcasted_iota(jnp.int32, s0.shape, 1) // rows

    def woven(base):
        turns = [(LANES - base) % LANES, (rows - base) % LANES, (2 * rows - base) % LANES]
        a = pltpu.roll(s0, turns[0], 1) if turns[0] else s0
        b = pltpu.roll(s1, turns[1], 1) if turns[1] else s1
        d = pltpu.roll(s0, turns[1], 1) if turns[1] else s0
        e = pltpu.roll(s1, turns[2], 1) if turns[2] else s1
        return jnp.where(spot == 0, a, jnp.where(spot == 1, b, jnp.where(spot == 2, d, e)))

    first_half, second_half = woven(0), woven(LANES // 2)
    for sub in range(subs):
        for part, lines in enumerate((first_half, second_half)):
            cols = pl.ds((2 * sub + part) * LANES, LANES)
            out_ref[:, cols] = (mix_t[:, cols] * lines[sub:sub + 1] * out_gain).astype(BF16)

    wait(own.at[pl.ds(0, chips - 1)], ag_send)
    wait(own_w.at[pl.ds(0, chips - 1)], agw_send)
    wait(own, dd_send)
    wait(own_w, ddw_send)
    wait(y_snd, y_send)
    wait(rs_s.at[pl.ds(0, (chips - 1) * subs)], rs_send)
    wait(mix.at[c], mix_send)
    wait(stat.at[pl.ds(0, chips - 1)], stat_send)
    wait(total.at[c], tot_send)


def solution(mesh):
    n_ep = mesh.shape["ep"]
    chips = n_ep // 2

    def per_device(
        tokens, routes, in_gain, group_router, expert_router, w_gate, w_up, w_down, out_gain
    ):
        rows, width = tokens.shape
        top = routes.shape[1]
        hidden = w_gate.shape[2]
        feats = out_gain.shape[0]
        half = chips // 2
        subs = 4
        all_rows = n_ep * rows
        block = 4 * rows
        dma, vmem = pltpu.SemaphoreType.DMA, pltpu.VMEM
        turned = pl.pallas_call(
            functools.partial(layer_kernel, n_ep),
            out_shape=jax.ShapeDtypeStruct((feats, all_rows), BF16),
            in_specs=[pl.BlockSpec(memory_space=pl.ANY)] * 9,
            out_specs=pl.BlockSpec(memory_space=vmem),
            scratch_shapes=[
                vmem((rows, width), BF16),
                vmem((top, rows), jnp.int32),
                vmem((1, width), F32),
                vmem((n_ep + 8, width), F32),
                vmem((1, feats), F32),
                vmem(w_gate.shape, BF16),
                vmem(w_up.shape, BF16),
                vmem(w_down.shape, BF16),
                vmem((chips, rows, width), BF16),
                vmem((chips, rows, width), BF16),
                vmem((chips, 8, LANES), F32),
                vmem((chips, 8, LANES), F32),
                vmem((block, hidden), F32),
                vmem((block, hidden), BF16),
                vmem((chips, rows, width), F32),
                vmem((chips, rows, width), BF16),
                vmem((chips, rows, width), BF16),
                vmem((chips * subs, chips // subs, rows, LANES), BF16),
                vmem((chips * subs, chips // subs, rows, LANES), BF16),
                vmem((2, chips, rows, LANES), F32),
                vmem((feats, all_rows), F32),
                vmem((chips, subs, LANES), F32),
                vmem((2, subs, LANES), F32),
                dma((6,)),
                dma((3,)),
                dma((2, half, subs)),
                dma((2, half)),
                dma((chips,)),
                dma((chips,)),
                dma,
                dma((chips * subs,)),
                dma,
                dma,
                dma,
            ] + [dma] * 9,
            compiler_params=pltpu.CompilerParams(collective_id=0, has_side_effects=True),
        )(
            tokens, routes.T, in_gain.reshape(1, width), group_router.T, expert_router.T,
            w_gate, w_up, w_down, out_gain.reshape(1, feats),
        )
        return turned.T

    in_specs = (
        P(("grp", "ep"), None),
        P(("grp", "ep"), None),
        P(),
        P(),
        P(),
        P("ep", None, None),
        P("ep", None, None),
        P("ep", None, None),
        P("ep"),
    )
    return jax.shard_map(
        per_device, mesh=mesh, in_specs=in_specs, out_specs=P("grp", "ep"), check_vma=False
    )
```
